32 devices in a mesh: grp: 2 (over y), ep: 8 (over z, x), tp: 2 (over core).
Axes of the slice: x: 2, y: 2, z: 4, core: 2. Of those that a mesh axis runs over, the one named last changes fastest.
Arguments:
- tokens: bfloat16 [4096, 2048], P(('grp', 'ep'), 'tp'), parts along dimension 0, may hold values from -6 to 6
- norm_gain: bfloat16 [2048], P('tp'), may hold values from 0.099609375 to 1.8984375
- w_gate: bfloat16 [8, 2048, 1024], P('ep', None, 'tp'), may hold values from -0.125 to 0.125
- w_up: bfloat16 [8, 2048, 1024], P('ep', None, 'tp'), may hold values from -0.125 to 0.125
- w_down: bfloat16 [8, 1024, 2048], P('ep', 'tp'), may hold values from -0.1875 to 0.1875
- expert_ids: int32 [4096, 2], P(('grp', 'ep')), parts along dimension 0, may hold values from 0 to 7, as said below
- combine: float32 [4096, 2], P(('grp', 'ep')), parts along dimension 0, may hold values from 0.1 to 1
- final_gain: bfloat16 [2048], P('tp'), may hold values from 0.099609375 to 1.8984375
Outputs:
- result: bfloat16 [4096, 2048], P(('grp', 'ep'), 'tp'), parts along dimension 0
The draws below stay inside these ranges and needn't reach their ends.
There are 2 independent parts, one for each index of `grp`. The reference program is written for one: setup_inputs(seed, part) draws one part's arguments, and reference() takes and returns one part's arrays. A program takes and returns all parts, laid end to end along the dimension named above; an argument that names none is the same for every part. Nothing has to cross between parts.
Inputs may be any that keep to these rules, and one draw needn't show every extreme that they name: `expert_ids`: the experts form 4 groups of consecutive ids of equal size; the 2 experts of a row are different and lie in one group. Among the rows of one index of ep no expert is named more than 160 times, and in each such block some expert is named exactly 160 times.
All inputs are finite; a program needn't handle non-finite values.
Results may differ from the reference program's by a relative error of at most 0.0077.
Values may be sent and summed in bfloat16 or wider, within the bound.
A program may use at most 64 MiB of HBM per device.

```python
import math
import jax
import jax.numpy as jnp
from jax import lax

D = 2048
FF = 1024
GROUPS = 4
TOP = 2
TOK_DEV = 256
EXPERTS = 8
CAP = 160
TOKENS = 2048
N_EP = 8
N_TP = 2


def draw_expert_ids(key, part):
    per_group = EXPERTS // GROUPS
    base = TOK_DEV // 8

    def one_block(block_key):
        key_busy, key_order, key_shift = jax.random.split(block_key, 3)
        busy = jax.random.randint(key_busy, (), 0, GROUPS)
        labels = jnp.arange(GROUPS, dtype=jnp.int32)
        counts = jnp.where(labels == busy, 5 * base, base).astype(jnp.int32)
        starts = jnp.cumsum(counts) - counts
        order = jax.random.permutation(key_order, TOK_DEV)
        ranks = jnp.arange(TOK_DEV, dtype=jnp.int32)
        group = jnp.sum((ranks[:, None] >= (starts + counts)[None, :]).astype(jnp.int32), axis=1)
        inner = ranks - starts[group]
        shifts = jax.random.randint(key_shift, (GROUPS,), 0, per_group)[group]
        first = (inner + shifts) % per_group
        second = (first + 1 + inner // per_group % max(per_group - 1, 1)) % per_group
        paired = jnp.stack([group * per_group + first, group * per_group + second], axis=1).astype(jnp.int32)
        return jnp.zeros((TOK_DEV, 2), jnp.int32).at[order].set(paired)
    blocks = jax.vmap(one_block)(jax.random.split(jax.random.fold_in(key, 11), TOKENS // TOK_DEV))
    return blocks.reshape(TOKENS, 2)


def block_scale(key, dims, cuts, low, high):
    loudness, own = 1.0, jax.random.fold_in(key, 6)
    for dim, blocks in cuts:
        steps = jnp.exp(jax.random.uniform(jax.random.fold_in(own, dim), (blocks,), jnp.float32, low / len(cuts), high / len(cuts)))
        loudness = loudness * jnp.repeat(steps, dims[dim] // blocks).reshape([-1 if axis == dim else 1 for axis in range(len(dims))])
    return loudness


def scatter_about(rng, dims, deviation, reach, cuts=(), held_as=jnp.bfloat16):
    array = deviation * jax.random.normal(rng, dims, jnp.float32)
    if cuts:
        array = array * block_scale(rng, dims, cuts, -0.22, 0.18)
    return jnp.clip(array, -reach, reach).astype(held_as)


def setup_inputs(seed: int = 0, part: int = 0) -> dict:
    key_of = jax.random.split(jax.random.key(seed), 9)
    own_keys = jax.random.split(jax.random.fold_in(key_of[8], part), 9)
    tokens = scatter_about(own_keys[0], (TOKENS, D), 1.0, 6.0, ((0, 8), (1, 2)))
    norm_gain = jnp.clip(1.0 + 0.18 * jax.random.normal(key_of[1], (D,), jnp.float32), 0.099609375, 1.8984375).astype(jnp.bfloat16)
    w_gate = scatter_about(key_of[2], (EXPERTS, D, FF), D ** -0.5, 0.125, ((0, 8), (2, 2)))
    w_up = scatter_about(key_of[3], (EXPERTS, D, FF), D ** -0.5, 0.125, ((0, 8), (2, 2)))
    w_down = scatter_about(key_of[4], (EXPERTS, FF, D), FF ** -0.5, 0.1875, ((0, 8), (1, 2)))
    expert_ids = draw_expert_ids(jax.random.fold_in(jax.random.fold_in(key_of[8], part), 71), part)
    combine = jnp.clip(jnp.exp(math.log(1.0) - 2.3025851 * jax.random.uniform(own_keys[6], (TOKENS, TOP), jnp.float32) ** block_scale(own_keys[6], (TOKENS, TOP), ((0, 8),), -0.2, 0.2)), 0.1, 1.0)
    final_gain = jnp.clip(1.0 + 0.18 * jax.random.normal(key_of[7], (D,), jnp.float32), 0.099609375, 1.8984375).astype(jnp.bfloat16)
    return dict(tokens=tokens, norm_gain=norm_gain, w_gate=w_gate, w_up=w_up, w_down=w_down, expert_ids=expert_ids, combine=combine, final_gain=final_gain)


def reference(tokens, norm_gain, w_gate, w_up, w_down, expert_ids, combine, final_gain):
    eps = 1e-06
    xf = tokens.astype(jnp.float32)
    normed = (xf * lax.rsqrt(lax.optimization_barrier(jnp.mean(xf * xf, axis=-1, keepdims=True)) + eps) * norm_gain.astype(jnp.float32)).astype(jnp.bfloat16)
    flat = expert_ids.reshape(-1)
    weights = combine.reshape(-1)
    limit = N_EP * CAP
    half_ff = FF // N_TP

    def step(acc, expert):
        hits = flat == expert
        pos = jnp.nonzero(hits, size=limit, fill_value=0)[0].astype(jnp.int32)
        live = jnp.arange(limit, dtype=jnp.int32) < jnp.sum(hits.astype(jnp.int32))
        owner = pos // TOP
        rows = normed[owner].astype(jnp.float32)
        gate_w = lax.dynamic_index_in_dim(w_gate, expert, 0, keepdims=False).astype(jnp.float32)
        up_w = lax.dynamic_index_in_dim(w_up, expert, 0, keepdims=False).astype(jnp.float32)
        down_w = lax.dynamic_index_in_dim(w_down, expert, 0, keepdims=False).astype(jnp.float32)
        gate = jnp.dot(rows, gate_w, preferred_element_type=jnp.float32)
        upper = jnp.dot(rows, up_w, preferred_element_type=jnp.float32)
        hidden = (jax.nn.silu(gate) * upper).astype(jnp.bfloat16)
        parts = jnp.einsum('rjf,jfd->jrd', hidden.astype(jnp.float32).reshape(limit, N_TP, half_ff), down_w.reshape(N_TP, half_ff, D)).astype(jnp.bfloat16)
        parts = lax.optimization_barrier(parts)
        summed = lax.optimization_barrier(jnp.sum(parts.astype(jnp.float32), axis=0)).astype(jnp.bfloat16)
        summed = lax.optimization_barrier(summed)
        scale = jnp.where(live, weights[pos], jnp.float32(0.0))
        acc = acc.at[owner].add(scale[:, None] * summed.astype(jnp.float32))
        return (acc, None)
    mixed, _ = lax.scan(step, jnp.zeros((TOKENS, D), jnp.float32), jnp.arange(EXPERTS, dtype=jnp.int32))
    norm = lax.rsqrt(lax.optimization_barrier(jnp.mean(mixed * mixed, axis=-1, keepdims=True)) + eps)
    return (mixed * norm * final_gain.astype(jnp.float32)).astype(jnp.bfloat16)
```

```python
import functools

import jax
import jax.numpy as jnp
from jax import lax
from jax.experimental import pallas as pl
from jax.experimental.pallas import tpu as pltpu
from jax.sharding import PartitionSpec as P

GROUPS = 4
EPS = 1e-06
MESH = pl.DeviceIdType.MESH
bf16, f32 = jnp.bfloat16, jnp.float32


def general(tokens, norm_gain, w_gate, w_up, w_down, expert_ids, combine, final_gain):
    eps = EPS
    tok_dev, half = tokens.shape
    n_ep = lax.axis_size("ep")
    n_tp = lax.axis_size("tp")
    width = half * n_tp
    exp_dev = w_gate.shape[0]
    experts = exp_dev * n_ep
    per_group = experts // GROUPS
    capacity = tok_dev // 8 * 5 * 2 // per_group
    top = expert_ids.shape[1]
    narrow = tokens.astype(jnp.float32)
    squares = lax.psum(jnp.sum(narrow * narrow, axis=1), "tp")
    scale = lax.rsqrt(squares[:, None] / width + eps)
    normed = (narrow * scale * norm_gain.astype(jnp.float32)).astype(jnp.bfloat16)
    columns = normed.shape[1]
    flat = expert_ids.reshape(-1)
    onehot = (flat[:, None] == jnp.arange(experts, dtype=jnp.int32)[None, :]).astype(jnp.int32)
    ranking = jnp.sum(jnp.cumsum(onehot, axis=0) * onehot, axis=1) - 1
    target = flat * capacity + ranking
    sources = jnp.arange(tok_dev * top, dtype=jnp.int32) // top
    owner = jnp.full((experts * capacity,), tok_dev, jnp.int32).at[target].set(sources)
    padded = jnp.concatenate([normed, jnp.zeros((1, columns), jnp.bfloat16)], axis=0)
    outgoing = padded[owner].reshape(n_ep, exp_dev * capacity, columns)
    arrived = lax.all_to_all(outgoing, "ep", split_axis=0, concat_axis=0, tiled=True)
    rows = (
        arrived.reshape(n_ep, exp_dev, capacity, columns)
        .transpose(1, 0, 2, 3)
        .reshape(exp_dev, n_ep * capacity, columns)
    )
    piece = lax.all_gather(rows, "tp", axis=2, tiled=True)
    gate = jnp.einsum("erd,edf->erf", piece, w_gate, preferred_element_type=jnp.float32)
    upper = jnp.einsum("erd,edf->erf", piece, w_up, preferred_element_type=jnp.float32)
    hidden = (jax.nn.silu(gate) * upper).astype(jnp.bfloat16)
    partial_out = jnp.einsum(
        "erf,efd->erd", hidden, w_down, preferred_element_type=jnp.float32
    ).astype(jnp.bfloat16)
    shares = (
        lax.psum_scatter(partial_out, "tp", scatter_dimension=2, tiled=True)
        .astype(jnp.float32)
        .astype(jnp.bfloat16)
    )
    homeward = (
        shares.reshape(exp_dev, n_ep, capacity, half)
        .transpose(1, 0, 2, 3)
        .reshape(n_ep, exp_dev * capacity, half)
    )
    returned = lax.all_to_all(homeward, "ep", split_axis=0, concat_axis=0, tiled=True).reshape(
        experts * capacity, half
    )
    picked = returned[target].astype(jnp.float32).reshape(tok_dev, top, half)
    mixed = jnp.sum(picked * combine[:, :, None], axis=1)
    totals = lax.psum(jnp.sum(mixed * mixed, axis=1), "tp")
    norm = lax.rsqrt(totals[:, None] / width + eps)
    return (mixed * norm * final_gain.astype(jnp.float32)).astype(jnp.bfloat16)


def fold(v):
    v = v * v
    out = v[:, :128]
    for i in range(1, v.shape[1] // 128):
        out = out + v[:, i * 128 : (i + 1) * 128]
    return out


def paired_kernel(
    G, cap, tok_ref, gain_ref, ids_ref, comb_ref, fgain_ref, wg_hbm, wu_hbm, wd_hbm, out_ref,
    wg, wu, wd, xbuf, sbuf, meta, psend, pown, precv, ebuf, xret, zbuf, ret, sq,
    wsem, sq_s, sq_r, z_s, z_r, m_s, m_r, x_s, x_r, t_s, t_r, p_s, p_r, e_s, e_r, h_s, h_r,
):
    rows, half = tok_ref.shape
    ep, c = lax.axis_index("ep"), lax.axis_index("tp")
    g, j = ep // 2, ep % 2
    other = {"ep": g * 2 + (1 - j)}
    core = {"tp": 1 - c}

    def plane(d):
        return {"ep": ((g + d + G) % G) * 2 + j}

    barrier = pltpu.get_barrier_semaphore()
    for dev in [core, other] + [plane(d) for d in range(1, G)]:
        pl.semaphore_signal(barrier, inc=1, device_id=dev, device_id_type=MESH)

    loads = []
    for i, h in enumerate((c, 1 - c)):
        at = pl.ds(pl.multiple_of(h * half, half), half)
        loads.append(pltpu.make_async_copy(wg_hbm.at[0, at, :], wg.at[i], wsem.at[i]))
        loads.append(pltpu.make_async_copy(wu_hbm.at[0, at, :], wu.at[i], wsem.at[2 + i]))
        loads.append(pltpu.make_async_copy(wd_hbm.at[0, :, at], wd.at[i], wsem.at[4 + i]))
    for load in loads:
        load.start()

    sent = []

    def send(src, dst, s, r, dev):
        copy = pltpu.make_async_remote_copy(
            src_ref=src, dst_ref=dst, send_sem=s, recv_sem=r, device_id=dev, device_id_type=MESH
        )
        copy.start()
        sent.append(copy)
        return copy

    x = tok_ref[...].astype(f32)
    sq[0] = fold(x)

    group = ids_ref[0:1, :] // 2
    slot8 = lax.broadcasted_iota(jnp.int32, (8, rows), 0)
    onehot = (slot8 == group).astype(f32)
    up_to = lax.broadcasted_iota(jnp.int32, (rows, rows), 0) <= lax.broadcasted_iota(
        jnp.int32, (rows, rows), 1
    )
    counted = jnp.dot(onehot.astype(bf16), up_to.astype(f32).astype(bf16), preferred_element_type=f32)
    rank = jnp.sum(onehot * counted, axis=0, keepdims=True) - 1.0
    offset = (group - g + G) % G
    target = offset * cap + rank.astype(jnp.int32)
    first = ids_ref[0:1, :] % 2 == 0
    c0, c1 = comb_ref[0:1, :], comb_ref[1:2, :]
    table = jnp.where(slot8 == 0, jnp.where(first, c0, c1), 0.0)
    table = jnp.where(slot8 == 1, jnp.where(first, c1, c0), table)
    table = jnp.where(slot8 == 2, rank, table)
    table = jnp.where(slot8 == 3, group.astype(f32), table)
    meta[0] = table
    pick = (lax.broadcasted_iota(jnp.int32, (G * cap, rows), 0) == target).astype(f32).astype(bf16)

    pl.semaphore_wait(barrier, 1 + G)
    first_sq = send(sq.at[0], sq.at[1], sq_s.at[0], sq_r.at[0], core)
    metas = [None] + [
        send(meta.at[0], meta.at[d], m_s.at[d], m_r.at[d], plane(d)) for d in range(1, G)
    ]
    first_sq.wait_recv()
    total = jnp.sum(sq[0] + sq[1], axis=1, keepdims=True)
    scale = lax.rsqrt(total / (2 * half) + EPS)
    normed = (x * scale * gain_ref[...].astype(f32)).astype(bf16)

    def gather(d):
        return jnp.dot(
            pick[d * cap : (d + 1) * cap], normed, preferred_element_type=f32
        ).astype(bf16)

    zs, xs, ts, fs, ps, es, hs = ([None] * G for _ in range(7))

    def arrived(d):
        if d:
            zs[d].wait_recv()
        xs[d] = send(xbuf.at[0, d, 0], xbuf.at[0, d, 1], x_s.at[d], x_r.at[d], other)
        ts[d] = send(xbuf.at[0, d, 0], xbuf.at[1, d, 0], t_s.at[d, 0], t_r.at[d, 0], core)

    def crossed(d):
        xs[d].wait_recv()
        fs[d] = send(xbuf.at[0, d, 1], xbuf.at[1, d, 1], t_s.at[d, 1], t_r.at[d, 1], core)

    def compute(d):
        ts[d].wait_recv()
        fs[d].wait_recv()
        a = xbuf[0, d].reshape(2 * cap, half)
        b = xbuf[1, d].reshape(2 * cap, half)
        gate = jnp.dot(a, wg[0], preferred_element_type=f32) + jnp.dot(
            b, wg[1], preferred_element_type=f32
        )
        upper = jnp.dot(a, wu[0], preferred_element_type=f32) + jnp.dot(
            b, wu[1], preferred_element_type=f32
        )
        hidden = (gate / (1.0 + jnp.exp(-gate)) * upper).astype(bf16)
        psend[d] = jnp.dot(hidden, wd[1], preferred_element_type=f32).astype(bf16).reshape(2, cap, half)
        ps[d] = send(psend.at[d], precv.at[d], p_s.at[d], p_r.at[d], core)
        pown[d] = jnp.dot(hidden, wd[0], preferred_element_type=f32).astype(bf16).reshape(2, cap, half)

    def summed(d):
        ps[d].wait_recv()
        ebuf[d, 1] = (pown[d, 1].astype(f32) + precv[d, 1].astype(f32)).astype(bf16)
        es[d] = send(ebuf.at[d, 1], xret.at[d], e_s.at[d], e_r.at[d], other)
        ebuf[d, 0] = (pown[d, 0].astype(f32) + precv[d, 0].astype(f32)).astype(bf16)

    def mix(d):
        if d:
            metas[d].wait_recv()
        tab = meta[d]
        slots = lax.broadcasted_iota(jnp.int32, (cap, rows), 0)
        here = (tab[2:3].astype(jnp.int32) == slots) & (tab[3:4].astype(jnp.int32) == g)
        mine = jnp.where(j == 0, tab[0:1], tab[1:2])
        theirs = jnp.where(j == 0, tab[1:2], tab[0:1])
        mine = jnp.sum(jnp.where(here, mine, 0.0), axis=1, keepdims=True)
        theirs = jnp.sum(jnp.where(here, theirs, 0.0), axis=1, keepdims=True)
        es[d].wait_recv()
        value = (mine * ebuf[d, 0].astype(f32) + theirs * xret[d].astype(f32)).astype(bf16)
        if d:
            zbuf[d] = value
            hs[d] = send(zbuf.at[d], ret.at[d], h_s.at[d], h_r.at[d], plane(-d))
        else:
            ret[0] = value

    for d in range(1, G):
        sbuf[d] = gather(d)
        zs[d] = send(sbuf.at[d], xbuf.at[0, d, 0], z_s.at[d], z_r.at[d], plane(d))
        if d == 1:
            xbuf[0, 0, 0] = gather(0)
            arrived(0)
    for load in loads:
        load.wait()
    for step in range(G + 1):
        if step + 1 < G:
            arrived(step + 1)
        if step < G:
            crossed(step)
            compute(step)
            summed(step)
        if step >= 1:
            mix(step - 1)

    eye = lax.broadcasted_iota(jnp.int32, (rows, rows), 0) == lax.broadcasted_iota(
        jnp.int32, (rows, rows), 1
    )
    back = jnp.sum(jnp.where(eye, target.astype(f32), 0.0), axis=1, keepdims=True).astype(jnp.int32)
    mixed = jnp.zeros((rows, half), f32)
    for d in range(G):
        if d:
            hs[d].wait_recv()
        place = lax.broadcasted_iota(jnp.int32, (rows, cap), 1) + d * cap == back
        mixed = mixed + jnp.dot(
            place.astype(f32).astype(bf16), ret[d], preferred_element_type=f32
        )
    sq[2] = fold(mixed)
    last_sq = send(sq.at[2], sq.at[3], sq_s.at[1], sq_r.at[1], core)
    last_sq.wait_recv()
    total = jnp.sum(sq[2] + sq[3], axis=1, keepdims=True)
    norm = lax.rsqrt(total / (2 * half) + EPS)
    out_ref[...] = (mixed * norm * fgain_ref[...].astype(f32)).astype(bf16)
    for copy in sent:
        copy.wait_send()


def paired(tokens, norm_gain, w_gate, w_up, w_down, expert_ids, combine, final_gain):
    rows, half = tokens.shape
    G = lax.axis_size("ep") // 2
    cap = rows // 8 * 5
    ff = w_gate.shape[2]
    vmem = pl.BlockSpec(memory_space=pltpu.VMEM)
    hbm = pl.BlockSpec(memory_space=pl.ANY)
    dma = pltpu.SemaphoreType.DMA
    return pl.pallas_call(
        functools.partial(paired_kernel, G, cap),
        out_shape=jax.ShapeDtypeStruct((rows, half), bf16),
        in_specs=[vmem] * 5 + [hbm] * 3,
        out_specs=vmem,
        scratch_shapes=[
            pltpu.VMEM((2, half, ff), bf16),
            pltpu.VMEM((2, half, ff), bf16),
            pltpu.VMEM((2, ff, half), bf16),
            pltpu.VMEM((2, G, 2, cap, half), bf16),
            pltpu.VMEM((G, cap, half), bf16),
            pltpu.VMEM((G, 8, rows), f32),
            pltpu.VMEM((G, 2, cap, half), bf16),
            pltpu.VMEM((G, 2, cap, half), bf16),
            pltpu.VMEM((G, 2, cap, half), bf16),
            pltpu.VMEM((G, 2, cap, half), bf16),
            pltpu.VMEM((G, cap, half), bf16),
            pltpu.VMEM((G, cap, half), bf16),
            pltpu.VMEM((G, cap, half), bf16),
            pltpu.VMEM((4, rows, 128), f32),
            dma((6,)),
            dma((2,)), dma((2,)),
            dma((G,)), dma((G,)),
            dma((G,)), dma((G,)),
            dma((G,)), dma((G,)),
            dma((G, 2)), dma((G, 2)),
            dma((G,)), dma((G,)),
            dma((G,)), dma((G,)),
            dma((G,)), dma((G,)),
        ],
        compiler_params=pltpu.CompilerParams(
            collective_id=0, has_side_effects=True, vmem_limit_bytes=60 * 1024 * 1024
        ),
        name="paired",
    )(
        tokens, norm_gain[None, :], expert_ids.T, combine.T, final_gain[None, :],
        w_gate, w_up, w_down,
    )


def body(tokens, norm_gain, w_gate, w_up, w_down, expert_ids, combine, final_gain):
    experts = w_gate.shape[0] * lax.axis_size("ep")
    per_group = experts // GROUPS
    args = (tokens, norm_gain, w_gate, w_up, w_down, expert_ids, combine, final_gain)
    if (
        per_group == expert_ids.shape[1] == 2
        and w_gate.shape[0] == 1
        and lax.axis_size("tp") == 2
        and GROUPS <= 8
    ):
        return paired(*args)
    return general(*args)


def solution(mesh):
    placed = (
        P(("grp", "ep"), "tp"),
        P("tp"),
        P("ep", None, "tp"),
        P("ep", None, "tp"),
        P("ep", "tp", None),
        P(("grp", "ep"), None),
        P(("grp", "ep"), None),
        P("tp"),
    )
    return jax.shard_map(
        body, mesh=mesh, in_specs=placed, out_specs=P(("grp", "ep"), "tp"), check_vma=False
    )
```

```python
import functools

import jax
import jax.numpy as jnp
from jax import lax
from jax.experimental import pallas as pl
from jax.experimental.pallas import tpu as pltpu
from jax.sharding import PartitionSpec as P

GROUPS = 4
EPS = 1e-06
LEAD = 1
MESH = pl.DeviceIdType.MESH
bf16, f32 = jnp.bfloat16, jnp.float32


def general(tokens, norm_gain, w_gate, w_up, w_down, expert_ids, combine, final_gain):
    eps = EPS
    tok_dev, half = tokens.shape
    n_ep = lax.axis_size("ep")
    n_tp = lax.axis_size("tp")
    width = half * n_tp
    exp_dev = w_gate.shape[0]
    experts = exp_dev * n_ep
    per_group = experts // GROUPS
    capacity = tok_dev // 8 * 5 * 2 // per_group
    top = expert_ids.shape[1]
    narrow = tokens.astype(jnp.float32)
    squares = lax.psum(jnp.sum(narrow * narrow, axis=1), "tp")
    scale = lax.rsqrt(squares[:, None] / width + eps)
    normed = (narrow * scale * norm_gain.astype(jnp.float32)).astype(jnp.bfloat16)
    columns = normed.shape[1]
    flat = expert_ids.reshape(-1)
    onehot = (flat[:, None] == jnp.arange(experts, dtype=jnp.int32)[None, :]).astype(jnp.int32)
    ranking = jnp.sum(jnp.cumsum(onehot, axis=0) * onehot, axis=1) - 1
    target = flat * capacity + ranking
    sources = jnp.arange(tok_dev * top, dtype=jnp.int32) // top
    owner = jnp.full((experts * capacity,), tok_dev, jnp.int32).at[target].set(sources)
    padded = jnp.concatenate([normed, jnp.zeros((1, columns), jnp.bfloat16)], axis=0)
    outgoing = padded[owner].reshape(n_ep, exp_dev * capacity, columns)
    arrived = lax.all_to_all(outgoing, "ep", split_axis=0, concat_axis=0, tiled=True)
    rows = (
        arrived.reshape(n_ep, exp_dev, capacity, columns)
        .transpose(1, 0, 2, 3)
        .reshape(exp_dev, n_ep * capacity, columns)
    )
    piece = lax.all_gather(rows, "tp", axis=2, tiled=True)
    gate = jnp.einsum("erd,edf->erf", piece, w_gate, preferred_element_type=jnp.float32)
    upper = jnp.einsum("erd,edf->erf", piece, w_up, preferred_element_type=jnp.float32)
    hidden = (jax.nn.silu(gate) * upper).astype(jnp.bfloat16)
    partial_out = jnp.einsum(
        "erf,efd->erd", hidden, w_down, preferred_element_type=jnp.float32
    ).astype(jnp.bfloat16)
    shares = (
        lax.psum_scatter(partial_out, "tp", scatter_dimension=2, tiled=True)
        .astype(jnp.float32)
        .astype(jnp.bfloat16)
    )
    homeward = (
        shares.reshape(exp_dev, n_ep, capacity, half)
        .transpose(1, 0, 2, 3)
        .reshape(n_ep, exp_dev * capacity, half)
    )
    returned = lax.all_to_all(homeward, "ep", split_axis=0, concat_axis=0, tiled=True).reshape(
        experts * capacity, half
    )
    picked = returned[target].astype(jnp.float32).reshape(tok_dev, top, half)
    mixed = jnp.sum(picked * combine[:, :, None], axis=1)
    totals = lax.psum(jnp.sum(mixed * mixed, axis=1), "tp")
    norm = lax.rsqrt(totals[:, None] / width + eps)
    return (mixed * norm * final_gain.astype(jnp.float32)).astype(jnp.bfloat16)


def fold(v):
    v = v * v
    out = v[:, :128]
    for i in range(1, v.shape[1] // 128):
        out = out + v[:, i * 128 : (i + 1) * 128]
    return out


def paired_kernel(
    G, cap, tok_ref, gain_ref, ids_ref, comb_ref, wg_hbm, wu_hbm, wd_hbm, out_ref,
    wg, wu, wd, xbuf, sbuf, meta, psend, pown, precv, ebuf, xret, zbuf, ret, sq,
    wsem, sq_s, sq_r, z_s, z_r, m_s, m_r, x_s, x_r, t_s, t_r, p_s, p_r, e_s, e_r, h_s, h_r,
):
    rows, half = tok_ref.shape
    ep, c = lax.axis_index("ep"), lax.axis_index("tp")
    g, j = ep // 2, ep % 2
    other = {"ep": g * 2 + (1 - j)}
    core = {"tp": 1 - c}

    cut = cap // 2

    def flip(a, d):
        return (a % 2 + d % 2) % 2 + 2 * ((a // 2 + d // 2) % 2)

    def plane(d):
        return {"ep": flip(g, d) * 2 + j}

    inner = ((g + 1) // 2) % 2
    order = [0, 1, 2 + inner, 3 - inner]

    barrier = pltpu.get_barrier_semaphore()
    for dev in [core, other] + [plane(d) for d in range(1, G)]:
        pl.semaphore_signal(barrier, inc=1, device_id=dev, device_id_type=MESH)

    loads = []
    for i, h in enumerate((c, 1 - c)):
        at = pl.ds(pl.multiple_of(h * half, half), half)
        loads.append(pltpu.make_async_copy(wg_hbm.at[0, at, :], wg.at[i], wsem.at[i]))
        loads.append(pltpu.make_async_copy(wu_hbm.at[0, at, :], wu.at[i], wsem.at[2 + i]))
        loads.append(pltpu.make_async_copy(wd_hbm.at[0, :, at], wd.at[i], wsem.at[4 + i]))
    for load in loads:
        load.start()

    sent = []

    def send(src, dst, s, r, dev):
        copy = pltpu.make_async_remote_copy(
            src_ref=src, dst_ref=dst, send_sem=s, recv_sem=r, device_id=dev, device_id_type=MESH
        )
        copy.start()
        sent.append(copy)
        return copy

    x = tok_ref[...].astype(f32)
    sq[0] = fold(x)

    group = ids_ref[0:1, :] // 2
    slot8 = lax.broadcasted_iota(jnp.int32, (8, rows), 0)
    onehot = (slot8 == group).astype(f32)
    up_to = lax.broadcasted_iota(jnp.int32, (rows, rows), 0) <= lax.broadcasted_iota(
        jnp.int32, (rows, rows), 1
    )
    counted = jnp.dot(onehot.astype(bf16), up_to.astype(f32).astype(bf16), preferred_element_type=f32)
    rank = jnp.sum(onehot * counted, axis=0, keepdims=True) - 1.0
    offset = flip(group, g)
    target = offset * cap + rank.astype(jnp.int32)
    first = ids_ref[0:1, :] % 2 == 0
    c0, c1 = comb_ref[0:1, :], comb_ref[1:2, :]
    table = jnp.where(slot8 == 0, jnp.where(first, c0, c1), 0.0)
    table = jnp.where(slot8 == 1, jnp.where(first, c1, c0), table)
    table = jnp.where(slot8 == 2, rank, table)
    table = jnp.where(slot8 == 3, group.astype(f32), table)
    meta[0] = table
    pick = (lax.broadcasted_iota(jnp.int32, (G * cap, rows), 0) == target).astype(f32).astype(bf16)

    pl.semaphore_wait(barrier, 1 + G)
    first_sq = send(sq.at[0], sq.at[1], sq_s.at[0], sq_r.at[0], core)
    metas = [None] + [
        send(meta.at[0], meta.at[d], m_s.at[d], m_r.at[d], plane(d)) for d in order[1:]
    ]
    first_sq.wait_recv()
    total = jnp.sum(sq[0] + sq[1], axis=1, keepdims=True)
    scale = lax.rsqrt(total / (2 * half) + EPS)
    normed = (x * scale * gain_ref[...].astype(f32)[None, :]).astype(bf16)

    def gather(d):
        return jnp.dot(
            pick[d * cap : (d + 1) * cap], normed, preferred_element_type=f32
        ).astype(bf16)

    units = [(d, r) for d in order for r in range(2)]
    U = len(units)
    zs, xs, ts, fs, ps, es, hs = ([None] * U for _ in range(7))

    def arrived(u):
        d, r = units[u]
        if zs[u] is not None:
            zs[u].wait_recv()
        mine = xbuf.at[0, d, r, 0]
        xs[u] = send(mine, xbuf.at[0, d, r, 1], x_s.at[d, r], x_r.at[d, r], other)
        ts[u] = send(mine, xbuf.at[1, d, r, 0], t_s.at[d, r, 0], t_r.at[d, r, 0], core)

    def crossed(u):
        d, r = units[u]
        xs[u].wait_recv()
        fs[u] = send(
            xbuf.at[0, d, r, 1], xbuf.at[1, d, r, 1], t_s.at[d, r, 1], t_r.at[d, r, 1], core
        )

    def compute(u):
        d, r = units[u]
        ts[u].wait_recv()
        fs[u].wait_recv()
        a = xbuf[0, d, r].reshape(2 * cut, half)
        b = xbuf[1, d, r].reshape(2 * cut, half)
        gate = jnp.dot(a, wg[0], preferred_element_type=f32) + jnp.dot(
            b, wg[1], preferred_element_type=f32
        )
        upper = jnp.dot(a, wu[0], preferred_element_type=f32) + jnp.dot(
            b, wu[1], preferred_element_type=f32
        )
        hidden = (gate / (1.0 + jnp.exp(-gate)) * upper).astype(bf16)
        away = jnp.dot(hidden, wd[1], preferred_element_type=f32)
        psend[d, r] = away.astype(bf16).reshape(2, cut, half)
        ps[u] = send(psend.at[d, r], precv.at[d, r], p_s.at[d, r], p_r.at[d, r], core)
        home = jnp.dot(hidden, wd[0], preferred_element_type=f32)
        pown[d, r] = home.astype(bf16).reshape(2, cut, half)

    def summed(u):
        d, r = units[u]
        ps[u].wait_recv()
        ebuf[d, r, 1] = (pown[d, r, 1].astype(f32) + precv[d, r, 1].astype(f32)).astype(bf16)
        es[u] = send(ebuf.at[d, r, 1], xret.at[d, r], e_s.at[d, r], e_r.at[d, r], other)
        ebuf[d, r, 0] = (pown[d, r, 0].astype(f32) + precv[d, r, 0].astype(f32)).astype(bf16)

    def mix(u):
        d, r = units[u]
        if u >= 2 and r == 0:
            metas[u // 2].wait_recv()
        tab = meta[d]
        slots = lax.broadcasted_iota(jnp.int32, (cut, rows), 0) + r * cut
        here = (tab[2:3].astype(jnp.int32) == slots) & (tab[3:4].astype(jnp.int32) == g)
        mine = jnp.where(j == 0, tab[0:1], tab[1:2])
        theirs = jnp.where(j == 0, tab[1:2], tab[0:1])
        mine = jnp.sum(jnp.where(here, mine, 0.0), axis=1, keepdims=True)
        theirs = jnp.sum(jnp.where(here, theirs, 0.0), axis=1, keepdims=True)
        es[u].wait_recv()
        value = (mine * ebuf[d, r, 0].astype(f32) + theirs * xret[d, r].astype(f32)).astype(bf16)
        if u >= 2:
            zbuf[d, r] = value
            hs[u] = send(zbuf.at[d, r], ret.at[d, r], h_s.at[d, r], h_r.at[d, r], plane(d))
        else:
            ret[0, r] = value

    def depart(u):
        d, r = units[u]
        zs[u] = send(sbuf.at[d, r], xbuf.at[0, d, r, 0], z_s.at[d, r], z_r.at[d, r], plane(d))

    sbuf[1] = gather(1).reshape(2, cut, half)
    depart(2)
    depart(3)
    own = gather(0).reshape(2, cut, half)
    for r in range(2):
        xbuf[0, 0, r, 0] = own[r]
        arrived(r)
    for d in range(2, G):
        sbuf[d] = gather(d).reshape(2, cut, half)
    for u in range(4, U):
        depart(u)
    for load in loads:
        load.wait()
    done = 2
    for u in range(U):
        while done < min(U, u + LEAD + 1):
            arrived(done)
            done += 1
        crossed(u)
        compute(u)
        summed(u)
        if u:
            mix(u - 1)
    mix(U - 1)

    eye = lax.broadcasted_iota(jnp.int32, (rows, rows), 0) == lax.broadcasted_iota(
        jnp.int32, (rows, rows), 1
    )
    back = jnp.sum(jnp.where(eye, target.astype(f32), 0.0), axis=1, keepdims=True).astype(jnp.int32)
    for copy in hs[2:]:
        copy.wait_recv()
    mixed = jnp.zeros((rows, half), f32)
    for d in range(G):
        place = lax.broadcasted_iota(jnp.int32, (rows, cap), 1) + d * cap == back
        mixed = mixed + jnp.dot(
            place.astype(f32).astype(bf16), ret[d].reshape(cap, half), preferred_element_type=f32
        )
    sq[2] = fold(mixed)
    last_sq = send(sq.at[2], sq.at[3], sq_s.at[1], sq_r.at[1], core)
    last_sq.wait_recv()
    total = jnp.sum(sq[2] + sq[3], axis=1, keepdims=True)
    norm = lax.rsqrt(total / (2 * half) + EPS)
    out_ref[...] = mixed * norm
    for copy in sent:
        copy.wait_send()


def paired(tokens, norm_gain, w_gate, w_up, w_down, expert_ids, combine, final_gain):
    rows, half = tokens.shape
    G = lax.axis_size("ep") // 2
    cap = rows // 8 * 5
    ff = w_gate.shape[2]
    vmem = pl.BlockSpec(memory_space=pltpu.VMEM)
    hbm = pl.BlockSpec(memory_space=pl.ANY)
    dma = pltpu.SemaphoreType.DMA
    out = pl.pallas_call(
        functools.partial(paired_kernel, G, cap),
        out_shape=jax.ShapeDtypeStruct((rows, half), f32),
        in_specs=[vmem] * 4 + [hbm] * 3,
        out_specs=vmem,
        scratch_shapes=[
            pltpu.VMEM((2, half, ff), bf16),
            pltpu.VMEM((2, half, ff), bf16),
            pltpu.VMEM((2, ff, half), bf16),
            pltpu.VMEM((2, G, 2, 2, cap // 2, half), bf16),
            pltpu.VMEM((G, 2, cap // 2, half), bf16),
            pltpu.VMEM((G, 8, rows), f32),
            pltpu.VMEM((G, 2, 2, cap // 2, half), bf16),
            pltpu.VMEM((G, 2, 2, cap // 2, half), bf16),
            pltpu.VMEM((G, 2, 2, cap // 2, half), bf16),
            pltpu.VMEM((G, 2, 2, cap // 2, half), bf16),
            pltpu.VMEM((G, 2, cap // 2, half), bf16),
            pltpu.VMEM((G, 2, cap // 2, half), bf16),
            pltpu.VMEM((G, 2, cap // 2, half), bf16),
            pltpu.VMEM((4, rows, 128), f32),
            dma((6,)),
            dma((2,)), dma((2,)),
            dma((G, 2)), dma((G, 2)),
            dma((G,)), dma((G,)),
            dma((G, 2)), dma((G, 2)),
            dma((G, 2, 2)), dma((G, 2, 2)),
            dma((G, 2)), dma((G, 2)),
            dma((G, 2)), dma((G, 2)),
            dma((G, 2)), dma((G, 2)),
        ],
        compiler_params=pltpu.CompilerParams(
            collective_id=0, has_side_effects=True, vmem_limit_bytes=60 * 1024 * 1024
        ),
        name="paired",
    )(
        tokens, norm_gain, expert_ids.T, combine.T, w_gate, w_up, w_down,
    )
    return (out * final_gain.astype(f32)).astype(bf16)


def body(tokens, norm_gain, w_gate, w_up, w_down, expert_ids, combine, final_gain):
    experts = w_gate.shape[0] * lax.axis_size("ep")
    per_group = experts // GROUPS
    args = (tokens, norm_gain, w_gate, w_up, w_down, expert_ids, combine, final_gain)
    if (
        per_group == expert_ids.shape[1] == 2
        and w_gate.shape[0] == 1
        and lax.axis_size("tp") == 2
        and GROUPS == 4
        and tokens.shape[0] % 256 == 0
    ):
        return paired(*args)
    return general(*args)


def solution(mesh):
    placed = (
        P(("grp", "ep"), "tp"),
        P("tp"),
        P("ep", None, "tp"),
        P("ep", None, "tp"),
        P("ep", "tp", None),
        P(("grp", "ep"), None),
        P(("grp", "ep"), None),
        P("tp"),
    )
    return jax.shard_map(
        body, mesh=mesh, in_specs=placed, out_specs=P(("grp", "ep"), "tp"), check_vma=False
    )
```
